32 devices in a mesh: ep: 8 (over z, x), tp: 4 (over y, core).
Axes of the slice: x: 2, y: 2, z: 4, core: 2. Of those that a mesh axis runs over, the one named last changes fastest.
Arguments:
- mixer_input: bfloat16 [4096, 2048], P('ep'), may hold values from -6 to 6
- mixer_gain: float32 [2048], replicated, may hold values from 0.1 to 1.9
- query_weight: bfloat16 [2048, 1024], P(None, 'tp'), may hold values from -0.125 to 0.125
- key_weight: bfloat16 [2048, 1024], P(None, 'tp'), may hold values from -0.125 to 0.125
- value_weight: bfloat16 [2048, 1024], P(None, 'tp'), may hold values from -0.125 to 0.125
- gate_weight: bfloat16 [2048, 1024], P(None, 'tp'), may hold values from -0.125 to 0.125
- head_gain: float32 [1024], P('tp'), may hold values from 0.1 to 1.9
- output_weight: bfloat16 [1024, 2048], P('tp'), may hold values from -0.1875 to 0.1875
- log_decay: float32 [4096, 8], P('ep', 'tp'), may hold values from -1 to 0, as said below
- expert_input: bfloat16 [4096, 2048], P(('ep', 'tp')), may hold values from -6 to 6
- expert_gain: float32 [2048], replicated, may hold values from 0.1 to 1.9
- routes: int32 [4096, 2], P(('ep', 'tp')), may hold values from 0 to 7, all different within a row; in each aligned block of 128 rows (0 to 127, 128 to 255, ...) at most 48 rows name the same one
- route_weight: float32 [4096, 2], P(('ep', 'tp')), may hold values from 0.1 to 1
- expert_gate: bfloat16 [8, 2048, 1024], P('ep', None, 'tp'), may hold values from -0.125 to 0.125
- expert_up: bfloat16 [8, 2048, 1024], P('ep', None, 'tp'), may hold values from -0.125 to 0.125
- expert_down: bfloat16 [8, 1024, 2048], P('ep', 'tp'), may hold values from -0.1875 to 0.1875
Outputs:
- mixer_output: bfloat16 [4096, 2048], P(('ep', 'tp'))
- expert_output: bfloat16 [4096, 2048], P(('ep', 'tp'))
The draws below stay inside these ranges and needn't reach their ends.
Inputs may be any that keep to these rules, and one draw needn't show every extreme that they name: `routes`: each row names 2 different experts. Among the rows of one device no expert is named more than 48 times, and in every draw the rows of some device name some expert exactly 48 times. `log_decay`: negative values.
All inputs are finite; a program needn't handle non-finite values.
Results may differ from the reference program's by a relative error of at most 0.025.
Values may be sent and summed in bfloat16 or wider, within the bound.
No kernel may reach another device: no remote copies, remote signals or barrier semaphores. Data moves between devices by JAX's collectives and lax.ppermute only.
A program may use at most 128 MiB of HBM per device.

```python
import math
import jax
import jax.numpy as jnp
import numpy as np
from jax import lax

D = 2048
HEADS = 8
HEAD_DIM = 128
FF = 1024
BLOCK = 128
TOPK = 2
TOK_A = 512
TOK_B = 128
RET_WIDTH = 1024
TOKENS_A = 4096
TOKENS_B = 4096
EXPERTS = 8
CAP = 48
N_EP = 8
N_TP = 4


def draw_log_decay(key, part):
    symbol_strings = jax.random.split(key, 7)
    series_extent = TOKENS_A
    fast_share = 50
    fast_heads = jax.random.randint(symbol_strings[0], (HEADS,), 0, 100) < fast_share
    fast_rate = 1.0 / jax.random.uniform(symbol_strings[1], (HEADS,), jnp.float32, 30.0, 60.0)
    slow_rate = 2.302585 * jax.random.uniform(symbol_strings[2], (HEADS,), jnp.float32, 0.3, 1.0) / (2.5 * series_extent)
    rate = jnp.where(fast_heads, fast_rate, slow_rate)
    shard_factor = jnp.repeat(jax.random.uniform(symbol_strings[3], (N_EP,), jnp.float32, 1.0, 2.5), TOK_A)
    rough = jax.random.uniform(symbol_strings[4], (series_extent, HEADS), jnp.float32, 0.5, 1.5)
    default_fading_exponent = -rate[None, :] * shard_factor[:, None] * rough
    spike_offset = jax.random.randint(symbol_strings[5], (3,), 0, series_extent)
    objective_scores = jax.random.uniform(symbol_strings[6], (3, HEADS), jnp.float32, 0.2, 0.4)
    agreeing_tally = (jnp.arange(series_extent, dtype=jnp.int32)[:, None] == spike_offset[None, :]).astype(jnp.float32)
    spike_clusters = jnp.sum(agreeing_tally[:, :, None] * jnp.log(1.0 - objective_scores)[None, :, :], axis=1)
    return (default_fading_exponent + spike_clusters).astype(jnp.float32)


def block_scale(key, extent, pieces, least, top_value):
    def one(dim, parts):
        heights = jax.random.uniform(jax.random.fold_in(jax.random.fold_in(key, 6), dim), (parts,), jnp.float32, least / len(pieces), top_value / len(pieces))
        return jnp.repeat(jnp.exp(heights), extent[dim] // parts).reshape((-1,) + (1,) * (len(extent) - dim - 1))

    loudness = one(*pieces[0])
    for cut in pieces[1:]:
        loudness = loudness * one(*cut)
    return loudness


def routed_block(own_key, own, number, rows, count, top, bound, lean):
    ranking = jax.random.permutation(own_key, count)
    packed, common = shares(count, rows * top, bound, lean, True), shares(count, rows * top, bound, lean, False)
    places = jnp.arange(count)

    def named(tallies, rotation):
        used = int((tallies > 0).sum())
        fixed = max(1, used // 4)
        moved = fixed + (places - fixed + rotation * (used - fixed)) % max(1, count - fixed)
        return jnp.zeros((count,), jnp.int32).at[ranking[jnp.where(places < fixed, places, moved)]].set(jnp.asarray(tallies, jnp.int32))

    tallies = jnp.where(number % 4 == 0, named(packed, number // 4), named(common, number - number // 4 - 1))
    mixed = jax.random.permutation(jax.random.fold_in(own, 3), count)
    donor, taker = mixed[0:count // 2 * 2:2], mixed[1:count // 2 * 2:2]
    margin = jnp.minimum(tallies[donor] - 1, bound - tallies[taker]) // 2
    margin = jnp.where((donor == ranking[0]) | (taker == ranking[0]) | (tallies[taker] == 0), 0, jnp.maximum(margin, 0))
    moved = jax.random.randint(jax.random.fold_in(own, 4), (count // 2,), 0, 1 << 20) % (margin + 1)
    tallies = tallies.at[donor].add(-moved).at[taker].add(moved)
    labels = jnp.searchsorted(jnp.cumsum(tallies), jnp.arange(rows * top), side="right").astype(jnp.int32)
    listing = labels.reshape(top, rows).T
    listing = listing[jax.random.permutation(jax.random.fold_in(own, 1), rows)]
    rotation = jax.random.randint(jax.random.fold_in(own, 2), (rows, 1), 0, top)
    return jnp.take_along_axis(listing, (jnp.arange(top)[None, :] + rotation) % top, axis=1)


def shares(number_of, total, most, skew, full):
    portions = [(1 << 20) // math.isqrt(standing ** skew) + 1 for standing in range(1, number_of + 1)]
    largest = most if full else min(most, max(-(-total // number_of), total * portions[0] // sum(portions)))
    least = 1 if total - largest >= number_of - 1 else 0
    given, spare = [largest] + [least] * (number_of - 1), total - largest - least * (number_of - 1)
    while spare > 0:
        candidates = [i for i in range(1, number_of) if given[i] < largest] or [i for i in range(1, number_of) if given[i] < most]
        mass, budget = sum([portions[i] for i in candidates]), spare
        for i in candidates:
            more = min(most - given[i], max(1, budget * portions[i] // mass), spare)
            given[i] = given[i] + more
            spare = spare - more
    return np.array(given)


def gaussian(rng, dims, deviation, most, pieces=(), held_as=jnp.bfloat16):
    values = deviation * jax.random.normal(rng, dims, jnp.float32)
    if pieces:
        values = values * block_scale(rng, dims, pieces, -0.22, 0.18)
    return jnp.clip(values, -most, most).astype(held_as)


def setup_inputs(seed: int = 0) -> dict:
    splits = jax.random.split(jax.random.key(seed), 17)
    mixer_input = gaussian(splits[0], (TOKENS_A, D), 1.0, 6.0, ((0, 8),))
    mixer_gain = jnp.clip(1.0 + 0.18 * jax.random.normal(splits[1], (D,), jnp.float32), 0.1, 1.9)
    query_weight = gaussian(splits[2], (D, RET_WIDTH), D ** -0.5, 0.125, ((1, 4),))
    key_weight = gaussian(splits[3], (D, RET_WIDTH), D ** -0.5, 0.125, ((1, 4),))
    value_weight = gaussian(splits[4], (D, RET_WIDTH), D ** -0.5, 0.125, ((1, 4),))
    gate_weight = gaussian(splits[5], (D, RET_WIDTH), D ** -0.5, 0.125, ((1, 4),))
    head_gain = jnp.clip(1.0 + 0.18 * jax.random.normal(splits[6], (RET_WIDTH,), jnp.float32), 0.1, 1.9)
    output_weight = gaussian(splits[7], (RET_WIDTH, D), RET_WIDTH ** -0.5, 0.1875, ((0, 4),))
    log_decay = draw_log_decay(jax.random.fold_in(splits[16], 71), 0)
    expert_input = gaussian(splits[9], (TOKENS_B, D), 1.0, 6.0, ((0, 32),))
    expert_gain = jnp.clip(1.0 + 0.18 * jax.random.normal(splits[10], (D,), jnp.float32), 0.1, 1.9)
    routes_keys = jax.random.split(jax.random.fold_in(splits[11], 1), TOKENS_B // TOK_B)
    routes_turns = jax.random.permutation(jax.random.fold_in(splits[11], 3), TOKENS_B // TOK_B)
    routes = jax.vmap(lambda own, number: routed_block(jax.random.fold_in(splits[11], 2), own, number, TOK_B, EXPERTS, TOPK, CAP, 1))(routes_keys, routes_turns).reshape((TOKENS_B, TOPK))
    route_weight = jnp.clip(0.1 + 0.9 * jax.random.uniform(splits[12], (TOKENS_B, TOPK), jnp.float32) ** block_scale(splits[12], (TOKENS_B, TOPK), ((0, 32),), -0.2, 0.2), 0.1, 1.0)
    expert_gate = gaussian(splits[13], (EXPERTS, D, FF), D ** -0.5, 0.125, ((0, 8), (2, 4)))
    expert_up = gaussian(splits[14], (EXPERTS, D, FF), D ** -0.5, 0.125, ((0, 8), (2, 4)))
    expert_down = gaussian(splits[15], (EXPERTS, FF, D), FF ** -0.5, 0.1875, ((0, 8), (1, 4)))
    return dict(mixer_input=mixer_input, mixer_gain=mixer_gain, query_weight=query_weight, key_weight=key_weight, value_weight=value_weight, gate_weight=gate_weight, head_gain=head_gain, output_weight=output_weight, log_decay=log_decay, expert_input=expert_input, expert_gain=expert_gain, routes=routes, route_weight=route_weight, expert_gate=expert_gate, expert_up=expert_up, expert_down=expert_down)


EPS = 1e-06
HIGH = lax.Precision.HIGHEST

def norm_rows(values, gain):
    floats = values.astype(jnp.float32)
    scale = lax.rsqrt(lax.optimization_barrier(jnp.mean(floats * floats, axis=-1, keepdims=True)) + EPS)
    return (floats * scale * gain).astype(jnp.bfloat16)

def rotate(values, position):
    half_dim = values.shape[-1] // 2
    frequency = 10000.0 ** (-jnp.arange(half_dim, dtype=jnp.float32) / half_dim)
    angles = position.astype(jnp.float32)[:, None] * frequency[None, :]
    cosine = jnp.cos(angles)[:, None, :]
    sine_part = jnp.sin(angles)[:, None, :]
    first_half = values[..., :half_dim]
    second = values[..., half_dim:]
    return jnp.concatenate([first_half * cosine - second * sine_part, first_half * sine_part + second * cosine], axis=-1)

def lifted(array):
    return lax.optimization_barrier(array).astype(jnp.float32)

def retain(q_rot, k_rot, values_new, log_decay):
    series_extent, head_count, head_dim = q_rot.shape
    block_count = series_extent // BLOCK
    row_ids = lax.broadcasted_iota(jnp.int32, (BLOCK, BLOCK), 0)
    col_ids = lax.broadcasted_iota(jnp.int32, (BLOCK, BLOCK), 1)
    lower_mask = col_ids <= row_ids
    triangle = lower_mask.astype(jnp.float32)

    def shaped(array):
        return array.reshape((block_count, BLOCK) + array.shape[1:])

    def advance(carry_state, inputs):
        q_block, k_block, v_block, step_block = inputs
        cumulative = jnp.einsum('ij,jh->hi', triangle, step_block, precision=HIGH)
        block_total = cumulative[:, -1]
        differences = cumulative[:, :, None] - cumulative[:, None, :]
        decays = jnp.where(lower_mask, jnp.exp(jnp.where(lower_mask, differences, 0.0)), 0.0)
        q_float = q_block.astype(jnp.float32)
        k_float = k_block.astype(jnp.float32)
        v_float = v_block.astype(jnp.float32)
        scores = jnp.einsum('ihd,jhd->hij', q_float, k_float, precision=HIGH)
        weights = lifted((scores * decays).astype(jnp.bfloat16))
        inner_term = jnp.einsum('hij,jhe->ihe', weights, v_float, precision=HIGH)
        cross_term = jnp.einsum('hi,ihd,hde->ihe', jnp.exp(cumulative), q_float, carry_state, precision=HIGH)
        key_scale = jnp.exp(block_total[:, None] - cumulative)
        updates = jnp.einsum('hj,jhd,jhe->hde', key_scale, k_float, v_float, precision=HIGH)
        next_state = jnp.exp(block_total)[:, None, None] * carry_state + updates
        return (next_state, inner_term + cross_term)
    initial = jnp.zeros((head_count, head_dim, head_dim), jnp.float32)
    _, outputs = lax.scan(advance, initial, (shaped(q_rot), shaped(k_rot), shaped(values_new), shaped(log_decay)))
    return outputs.reshape(series_extent, head_count, head_dim)

def reference(mixer_input, mixer_gain, query_weight, key_weight, value_weight, gate_weight, head_gain, output_weight, log_decay, expert_input, expert_gain, routes, route_weight, expert_gate, expert_up, expert_down):
    series_extent = mixer_input.shape[0]
    normed = norm_rows(mixer_input, mixer_gain)

    def project(weight):
        return jnp.dot(normed, weight, preferred_element_type=jnp.float32).astype(jnp.bfloat16)
    queries = project(query_weight)
    keys_raw = project(key_weight)
    values_new = project(value_weight)
    gate_raw = project(gate_weight)
    position = jnp.arange(series_extent, dtype=jnp.int32)
    q_rot = rotate(lifted(queries).reshape(series_extent, HEADS, HEAD_DIM), position).astype(jnp.bfloat16)
    k_rot = (rotate(lifted(keys_raw).reshape(series_extent, HEADS, HEAD_DIM), position) * HEAD_DIM ** (-0.5)).astype(jnp.bfloat16)
    retained = retain(q_rot, k_rot, values_new.reshape(series_extent, HEADS, HEAD_DIM), log_decay)
    centre = lax.optimization_barrier(jnp.mean(retained, axis=-1, keepdims=True))
    spread = lax.optimization_barrier(jnp.mean(jnp.square(retained - centre), axis=-1, keepdims=True))
    scaled = (retained - centre) * lax.rsqrt(spread + EPS) * head_gain.reshape(HEADS, HEAD_DIM)
    gated = scaled.reshape(series_extent, RET_WIDTH) * jax.nn.silu(lifted(gate_raw))
    mixer_hidden = gated.astype(jnp.bfloat16)
    quarter = RET_WIDTH // N_TP
    running = jnp.zeros((series_extent, D), jnp.float32)
    for group_index in range(N_TP):
        group_term = jnp.dot(mixer_hidden[:, group_index * quarter:(group_index + 1) * quarter], output_weight[group_index * quarter:(group_index + 1) * quarter], preferred_element_type=jnp.float32)
        running = running + lifted(group_term.astype(jnp.bfloat16))
    mixer_output = running.astype(jnp.bfloat16)
    expert_normed = norm_rows(expert_input, expert_gain)
    block_count = N_EP * N_TP
    entry_count = TOK_B * TOPK
    flat_routes = routes.reshape(block_count, entry_count)
    onehot = (flat_routes[:, :, None] == jnp.arange(EXPERTS, dtype=jnp.int32)[None, None, :]).astype(jnp.int32)
    prior_count = jnp.cumsum(onehot, axis=1) - onehot
    slot_index = lax.optimization_barrier(jnp.sum(prior_count * onehot, axis=2)).astype(jnp.int32)
    block_ids = jnp.broadcast_to(jnp.arange(block_count, dtype=jnp.int32)[:, None], (block_count, entry_count))
    entry_ids = block_ids * entry_count + jnp.arange(entry_count, dtype=jnp.int32)[None, :]
    slot_table = jnp.full((EXPERTS, block_count, CAP), -1, jnp.int32).at[flat_routes, block_ids, slot_index].set(entry_ids)
    norm_weight = route_weight / lax.optimization_barrier(jnp.sum(route_weight, axis=1, keepdims=True))
    flat_weight = norm_weight.reshape(-1)

    def per_expert(running_sum, inputs):
        gate_w, up_w, down_w, id_table = inputs
        id_list = id_table.reshape(-1)
        valid = id_list >= 0
        safe_ids = jnp.where(valid, id_list, 0).astype(jnp.int32)
        tok_index = (safe_ids // TOPK).astype(jnp.int32)
        rows_in = jnp.where(valid[:, None], expert_normed[tok_index], jnp.zeros((), jnp.bfloat16))
        gate_part = jnp.dot(rows_in, gate_w, preferred_element_type=jnp.float32)
        up_part = jnp.dot(rows_in, up_w, preferred_element_type=jnp.float32)
        hidden = (jax.nn.silu(gate_part) * up_part).astype(jnp.bfloat16)
        result = lifted(jnp.dot(hidden, down_w, preferred_element_type=jnp.float32).astype(jnp.bfloat16))
        scale = jnp.where(valid, flat_weight[safe_ids], 0.0)
        return (running_sum.at[tok_index].add(scale[:, None] * result), None)
    total, _ = lax.scan(per_expert, jnp.zeros((TOKENS_B, D), jnp.float32), (expert_gate, expert_up, expert_down, slot_table))
    expert_output = total.astype(jnp.bfloat16)
    return (mixer_output, expert_output)
```

```python
import functools

import jax
import jax.numpy as jnp
from jax import lax
from jax.experimental import pallas as pl
from jax.experimental.pallas import tpu as pltpu
from jax.sharding import PartitionSpec as P

BLOCK = 128
EPS = 1e-06
HIGH = lax.Precision.HIGHEST
PAD = 16
F32 = jnp.float32
BF16 = jnp.bfloat16


def dot(a, b, contract=((1,), (0,)), precision=None):
    return lax.dot_general(
        a, b, (contract, ((), ())), preferred_element_type=F32, precision=precision
    )


def normed_rows(values, gain):
    floats = values.astype(F32)
    scale = lax.rsqrt(jnp.mean(floats * floats, axis=-1, keepdims=True) + EPS)
    return (floats * scale * gain).astype(BF16)


def silu(v):
    return v / (1.0 + jnp.exp(-v))


def retain_kernel(
    x_ref,
    gain_ref,
    wq_ref,
    wk_ref,
    wv_ref,
    wg_ref,
    cos_ref,
    sin_ref,
    ld_ref,
    ldt_ref,
    ret_ref,
    qd_ref,
    gate_ref,
    pkg_ref,
    normed_ref,
    *,
    heads,
    head_dim,
):
    rows = x_ref.shape[0]
    blocks = rows // BLOCK
    for b in range(blocks):
        part = slice(b * BLOCK, (b + 1) * BLOCK)
        normed_ref[part, :] = normed_rows(x_ref[part, :], gain_ref[...])
    normed = normed_ref[...]
    q_all = dot(normed, wq_ref[...]).astype(BF16)
    k_all = dot(normed, wk_ref[...]).astype(BF16)
    v_all = dot(normed, wv_ref[...]).astype(BF16)
    gate_ref[...] = dot(normed, wg_ref[...]).astype(BF16)
    row_ids = lax.broadcasted_iota(jnp.int32, (BLOCK, BLOCK), 0)
    col_ids = lax.broadcasted_iota(jnp.int32, (BLOCK, BLOCK), 1)
    lower = col_ids <= row_ids
    tri = lower.astype(F32)
    tri_t = (row_ids <= col_ids).astype(F32)
    states = [jnp.zeros((head_dim, head_dim), F32) for _ in range(heads)]
    base = [jnp.zeros((1, 1), F32) for _ in range(heads)]
    for b in range(blocks):
        part = slice(b * BLOCK, (b + 1) * BLOCK)
        c_cols = dot(tri, ld_ref[part, :], precision=HIGH)
        c_rows = dot(ldt_ref[:, part], tri_t, precision=HIGH)
        cosine, sine = cos_ref[part, :], sin_ref[part, :]
        for h in range(heads):
            lanes = slice(h * head_dim, (h + 1) * head_dim)
            c_col = c_cols[:, h : h + 1]
            c_row = c_rows[h : h + 1, :]
            total = c_row[:, BLOCK - 1 : BLOCK]
            q = q_all[part, lanes].astype(F32)
            k = k_all[part, lanes].astype(F32)
            v = v_all[part, lanes]
            q = (q * cosine + pltpu.roll(q, head_dim // 2, 1) * sine).astype(BF16)
            k = (k * cosine + pltpu.roll(k, head_dim // 2, 1) * sine) * head_dim ** (-0.5)
            k = k.astype(BF16)
            decays = jnp.where(lower, jnp.exp(jnp.where(lower, c_col - c_row, 0.0)), 0.0)
            weights = (dot(q, k, ((1,), (1,))) * decays).astype(BF16)
            qf = q.astype(F32)
            inner = dot(weights, v)
            if b:
                inner = inner + dot((qf * jnp.exp(c_col)).astype(BF16), states[h].astype(BF16))
            ret_ref[part, lanes] = inner
            qd_ref[part, lanes] = (qf * jnp.exp(c_col + base[h])).astype(BF16)
            scaled = (k.astype(F32) * jnp.exp(total - c_col)).astype(BF16)
            update = dot(scaled, v, ((0,), (0,)))
            states[h] = jnp.exp(total) * states[h] + update
            base[h] = base[h] + total
    span = head_dim + PAD
    for h in range(heads):
        pkg_ref[h * span : h * span + head_dim, :] = states[h].astype(BF16)
        pkg_ref[h * span + head_dim : (h + 1) * span, :] = jnp.broadcast_to(
            jnp.exp(base[h]), (PAD, head_dim)
        ).astype(BF16)


def finish_kernel(index_ref, ret_ref, qd_ref, gate_ref, hgain_ref, wo_ref, *refs, heads, head_dim, count, pieces):
    packages, outs, hidden_ref = refs[:count], refs[count : count + pieces], refs[-1]
    span = head_dim + PAD
    for h in range(heads):
        lanes = slice(h * head_dim, (h + 1) * head_dim)
        state = jnp.zeros((head_dim, head_dim), F32)
        for package in reversed(packages):
            local = package[h * span : h * span + head_dim, :].astype(F32)
            factor = package[h * span + head_dim : (h + 1) * span, :].astype(F32)[0:1, :]
            state = factor * state + local
        kept = ret_ref[:, lanes] + dot(qd_ref[:, lanes], state.astype(BF16))
        centre = jnp.mean(kept, axis=-1, keepdims=True)
        away = kept - centre
        spread = jnp.mean(away * away, axis=-1, keepdims=True)
        scaled = away * lax.rsqrt(spread + EPS) * hgain_ref[:, lanes]
        hidden_ref[:, lanes] = (scaled * silu(gate_ref[:, lanes].astype(F32))).astype(BF16)
    for j in reversed(range(pieces)):
        size = outs[j].shape[0]
        start = pl.multiple_of(index_ref[j] * size, size)
        outs[j][...] = dot(hidden_ref[pl.ds(start, size), :], wo_ref[...]).astype(BF16)


def dispatch_kernel(x_ref, gain_ref, routes_ref, weight_ref, out_ref, hi_ref, lo_ref, *, capacity):
    tokens, top = routes_ref.shape
    slots = out_ref.shape[0]
    normed = normed_rows(x_ref[...], gain_ref[...])
    row_ids = lax.broadcasted_iota(jnp.int32, (tokens, tokens), 0)
    col_ids = lax.broadcasted_iota(jnp.int32, (tokens, tokens), 1)
    before = (col_ids < row_ids).astype(F32).astype(BF16)
    lane = lax.broadcasted_iota(jnp.int32, (tokens, 128), 1)
    slot = lax.broadcasted_iota(jnp.int32, (tokens, slots), 1)
    routes = routes_ref[...]
    scores = weight_ref[...]
    share = scores / jnp.sum(scores, axis=1, keepdims=True)
    offset = jnp.zeros((1, 128), F32)
    place = jnp.zeros((tokens, slots), F32)
    mix = jnp.zeros((tokens, slots), F32)
    for t in range(top):
        expert = routes[:, t : t + 1]
        onehot = (lane == expert).astype(F32)
        prior = dot(before, onehot.astype(BF16)) + offset
        position = jnp.sum(prior * onehot, axis=1, keepdims=True)
        target = expert * capacity + position.astype(jnp.int32)
        hit = (slot == target).astype(F32)
        place = place + hit
        mix = mix + hit * share[:, t : t + 1]
        offset = offset + jnp.sum(onehot, axis=0, keepdims=True)
    out_ref[...] = dot(place.astype(BF16), normed, ((0,), (0,))).astype(BF16)
    high = mix.astype(BF16)
    hi_ref[...] = high
    lo_ref[...] = (mix - high.astype(F32)).astype(BF16)


def gate_up_kernel(rows_ref, *refs, pieces):
    gates, ups = refs[:pieces], refs[pieces : 2 * pieces]
    out_ref, gacc_ref, uacc_ref = refs[2 * pieces :]
    step = pl.program_id(0)
    rows = rows_ref[...]
    width = gates[0].shape[1]

    @pl.when(step == 0)
    def _():
        gacc_ref[...] = jnp.zeros_like(gacc_ref)
        uacc_ref[...] = jnp.zeros_like(uacc_ref)

    for i in range(pieces):
        lanes = slice(i * width, (i + 1) * width)
        gacc_ref[:, lanes] += dot(rows, gates[i][...])
        uacc_ref[:, lanes] += dot(rows, ups[i][...])

    @pl.when(step == pl.num_programs(0) - 1)
    def _():
        out_ref[...] = (silu(gacc_ref[...]) * uacc_ref[...]).astype(BF16)


def gate_up(rows, gates, ups):
    count, width = rows.shape
    pieces, cols = len(gates), gates[0].shape[1]
    part = width // 4
    weight = pl.BlockSpec((part, cols), lambda i: (i, 0))
    return pl.pallas_call(
        functools.partial(gate_up_kernel, pieces=pieces),
        grid=(4,),
        in_specs=[pl.BlockSpec((count, part), lambda i: (0, i))] + [weight] * (2 * pieces),
        out_specs=pl.BlockSpec((count, pieces * cols), lambda i: (0, 0)),
        out_shape=jax.ShapeDtypeStruct((count, pieces * cols), BF16),
        scratch_shapes=[pltpu.VMEM((count, pieces * cols), F32)] * 2,
        name="gate_up",
    )(rows, *gates, *ups)


def down_kernel(*refs, groups):
    hiddens, downs, out_ref = refs[: len(groups)], refs[len(groups) : -1], refs[-1]
    total, at = None, 0
    for hidden, pieces in zip(hiddens, groups):
        cols = downs[at].shape[0]
        for i in range(pieces):
            term = dot(hidden[:, i * cols : (i + 1) * cols], downs[at][...])
            total = term if total is None else total + term
            at += 1
    out_ref[...] = total.astype(BF16)


def down(hiddens, groups):
    count = hiddens[0].shape[0]
    flat = [d for g in groups for d in g]
    inner, width = flat[0].shape
    part = width // 4
    return pl.pallas_call(
        functools.partial(down_kernel, groups=tuple(len(g) for g in groups)),
        grid=(4,),
        in_specs=[pl.BlockSpec(h.shape, lambda i: (0, 0)) for h in hiddens]
        + [pl.BlockSpec((inner, part), lambda i: (0, i))] * len(flat),
        out_specs=pl.BlockSpec((count, part), lambda i: (0, i)),
        out_shape=jax.ShapeDtypeStruct((count, width), BF16),
        name="down",
    )(*hiddens, *flat)


def combine_kernel(hi_ref, lo_ref, rows_ref, out_ref):
    rows = rows_ref[...]
    out_ref[...] = (dot(hi_ref[...], rows) + dot(lo_ref[...], rows)).astype(BF16)


def swap(x, axis, bit):
    return lax.ppermute(x, axis, [(i, i ^ bit) for i in range(lax.axis_size(axis))])


def entering_packages(package, heads, head_dim):
    peers = lax.axis_size("ep")
    if peers <= 8:
        return [
            lax.ppermute(package, "ep", [(i, i + k) for i in range(peers - k)])
            for k in range(1, peers)
        ]
    position = lax.axis_index("ep")
    span = head_dim + PAD
    everything = lax.all_gather(package, "ep").reshape(peers, heads, span, head_dim)

    def turn(k, before):
        part = everything[k].astype(F32)
        new = part[:, head_dim : head_dim + 1, :] * before + part[:, :head_dim, :]
        return jnp.where(k < position, new, before)

    state = lax.fori_loop(0, peers, turn, jnp.zeros((heads, head_dim, head_dim), F32))
    padded = jnp.pad(state, ((0, 0), (0, PAD), (0, 0))).astype(BF16)
    return [padded.reshape(heads * span, head_dim)]


def on_device(
    mixer_input,
    mixer_gain,
    query_weight,
    key_weight,
    value_weight,
    gate_weight,
    head_gain,
    output_weight,
    log_decay,
    expert_input,
    expert_gain,
    routes,
    route_weight,
    expert_gate,
    expert_up,
    expert_down,
):
    tp = lax.axis_size("tp")
    bits = []
    while (1 << len(bits)) < tp:
        bits.append(1 << len(bits))

    def spread(piece):
        pieces = [piece]
        for bit in reversed(bits):
            pieces = pieces + [swap(p, "tp", bit) for p in pieces]
        return pieces

    gates, ups, downs = spread(expert_gate[0]), spread(expert_up[0]), spread(expert_down[0])

    tokens, top = routes.shape
    experts = lax.axis_size("ep")
    capacity = max(2, 3 * tokens * top // (2 * experts))
    slots = experts * capacity
    width = expert_input.shape[1]
    outgoing, mix_hi, mix_lo = pl.pallas_call(
        functools.partial(dispatch_kernel, capacity=capacity),
        out_shape=(
            jax.ShapeDtypeStruct((slots, width), BF16),
            jax.ShapeDtypeStruct((tokens, slots), BF16),
            jax.ShapeDtypeStruct((tokens, slots), BF16),
        ),
        name="dispatch",
    )(expert_input, expert_gain.reshape(1, -1), routes, route_weight)
    arrived = lax.all_to_all(
        outgoing.reshape(experts, capacity, width), "ep", split_axis=0, concat_axis=0, tiled=True
    ).reshape(slots, width)

    rows = mixer_input.shape[0]
    heads = log_decay.shape[1]
    mix_width = query_weight.shape[1]
    head_dim = mix_width // heads
    half = head_dim // 2
    position = lax.axis_index("ep") * rows + jnp.arange(rows, dtype=jnp.int32)
    frequency = 10000.0 ** (-jnp.arange(half, dtype=F32) / half)
    angles = position.astype(F32)[:, None] * frequency[None, :]
    cosine, sine = jnp.cos(angles), jnp.sin(angles)
    cosine = jnp.concatenate([cosine, cosine], axis=1)
    sine = jnp.concatenate([-sine, sine], axis=1)
    decay_cols = jnp.pad(log_decay, ((0, 0), (0, 128 - heads)))
    decay_rows = jnp.pad(log_decay.T, ((0, 8 - heads), (0, 0)))
    span = head_dim + PAD
    retained, queries, gate_raw, package = pl.pallas_call(
        functools.partial(retain_kernel, heads=heads, head_dim=head_dim),
        out_shape=(
            jax.ShapeDtypeStruct((rows, mix_width), F32),
            jax.ShapeDtypeStruct((rows, mix_width), BF16),
            jax.ShapeDtypeStruct((rows, mix_width), BF16),
            jax.ShapeDtypeStruct((heads * span, head_dim), BF16),
        ),
        scratch_shapes=[pltpu.VMEM(mixer_input.shape, BF16)],
        name="retain",
    )(
        mixer_input,
        mixer_gain.reshape(1, -1),
        query_weight,
        key_weight,
        value_weight,
        gate_weight,
        cosine,
        sine,
        decay_cols,
        decay_rows,
    )
    packages = entering_packages(package, heads, head_dim)
    out_width = output_weight.shape[1]
    order = (lax.axis_index("tp") ^ jnp.arange(tp, dtype=jnp.int32)).astype(jnp.int32)
    vmem = pl.BlockSpec(memory_space=pltpu.VMEM)
    parts = pl.pallas_call(
        functools.partial(
            finish_kernel, heads=heads, head_dim=head_dim, count=len(packages), pieces=tp
        ),
        in_specs=[pl.BlockSpec(memory_space=pltpu.SMEM)] + [vmem] * (5 + len(packages)),
        out_specs=[vmem] * tp,
        out_shape=[jax.ShapeDtypeStruct((rows // tp, out_width), BF16)] * tp,
        scratch_shapes=[pltpu.VMEM((rows, mix_width), BF16)],
        name="finish",
    )(order, retained, queries, gate_raw, head_gain.reshape(1, -1), output_weight, *packages)
    sums = [part for part in parts]
    for bit in bits:
        kept = range(0, len(sums), 2 * bit)
        for j in kept:
            other = swap(sums[j + bit].astype(BF16), "tp", bit)
            sums[j] = sums[j].astype(F32) + other.astype(F32)
    mixer_output = sums[0].astype(BF16)

    near, far = slice(0, None, 2), slice(1, None, 2)
    if tp > 2:
        split = [near, far]
    else:
        split = [slice(0, None)]
    hiddens = [gate_up(arrived, gates[s], ups[s]) for s in split]
    results = down(hiddens, [downs[s] for s in split])
    returned = lax.all_to_all(
        results.reshape(experts, capacity, width), "ep", split_axis=0, concat_axis=0, tiled=True
    ).reshape(slots, width)
    expert_output = pl.pallas_call(
        combine_kernel,
        out_shape=jax.ShapeDtypeStruct((tokens, width), BF16),
        name="combine",
    )(mix_hi, mix_lo, returned)
    return (mixer_output, expert_output)


def solution(mesh):
    return jax.shard_map(
        on_device,
        mesh=mesh,
        in_specs=(
            P("ep", None),
            P(),
            P(None, "tp"),
            P(None, "tp"),
            P(None, "tp"),
            P(None, "tp"),
            P("tp"),
            P("tp", None),
            P("ep", "tp"),
            P(("ep", "tp"), None),
            P(),
            P(("ep", "tp"), None),
            P(("ep", "tp"), None),
            P("ep", None, "tp"),
            P("ep", None, "tp"),
            P("ep", "tp", None),
        ),
        out_specs=(P(("ep", "tp"), None), P(("ep", "tp"), None)),
        check_vma=False,
    )
```

```python
import functools

import jax
import jax.numpy as jnp
from jax import lax
from jax.experimental import pallas as pl
from jax.experimental.pallas import tpu as pltpu
from jax.sharding import PartitionSpec as P


BLOCK = 128
EPS = 1e-06
HIGH = lax.Precision.HIGHEST
PAD = 16
F32 = jnp.float32
BF16 = jnp.bfloat16


def dot(a, b, contract=((1,), (0,)), precision=None):
    return lax.dot_general(
        a, b, (contract, ((), ())), preferred_element_type=F32, precision=precision
    )


def normed_rows(values, gain):
    floats = values.astype(F32)
    scale = lax.rsqrt(jnp.mean(floats * floats, axis=-1, keepdims=True) + EPS)
    return (floats * scale * gain).astype(BF16)


def silu(v):
    return v / (1.0 + jnp.exp(-v))


def retain_kernel(
    x_ref,
    gain_ref,
    wq_ref,
    wk_ref,
    wv_ref,
    wg_ref,
    cos_ref,
    sin_ref,
    ldt_ref,
    ret_ref,
    qd_ref,
    gate_ref,
    pkg_ref,
    normed_ref,
    *,
    heads,
    head_dim,
):
    rows = x_ref.shape[0]
    blocks = rows // BLOCK
    for b in range(blocks):
        part = slice(b * BLOCK, (b + 1) * BLOCK)
        normed_ref[part, :] = normed_rows(x_ref[part, :], gain_ref[...])
    normed = normed_ref[...]
    q_all = dot(normed, wq_ref[...]).astype(BF16)
    k_all = dot(normed, wk_ref[...]).astype(BF16)
    v_all = dot(normed, wv_ref[...]).astype(BF16)
    gate_ref[...] = dot(normed, wg_ref[...]).astype(BF16)
    row_ids = lax.broadcasted_iota(jnp.int32, (BLOCK, BLOCK), 0)
    col_ids = lax.broadcasted_iota(jnp.int32, (BLOCK, BLOCK), 1)
    lower = col_ids <= row_ids
    tri = lower.astype(F32)
    tri_t = (row_ids <= col_ids).astype(F32)
    states = [jnp.zeros((head_dim, head_dim), F32) for _ in range(heads)]
    base = [jnp.zeros((1, 1), F32) for _ in range(heads)]
    for b in range(blocks):
        part = slice(b * BLOCK, (b + 1) * BLOCK)
        c_cols = dot(tri, ldt_ref[:, part], ((1,), (1,)), precision=HIGH)
        c_rows = dot(ldt_ref[:, part], tri_t, precision=HIGH)
        cosine, sine = cos_ref[part, :], sin_ref[part, :]
        for h in range(heads):
            lanes = slice(h * head_dim, (h + 1) * head_dim)
            c_col = c_cols[:, h : h + 1]
            c_row = c_rows[h : h + 1, :]
            total = c_row[:, BLOCK - 1 : BLOCK]
            q = q_all[part, lanes].astype(F32)
            k = k_all[part, lanes].astype(F32)
            v = v_all[part, lanes]
            q = (q * cosine + pltpu.roll(q, head_dim // 2, 1) * sine).astype(BF16)
            k = (k * cosine + pltpu.roll(k, head_dim // 2, 1) * sine) * head_dim ** (-0.5)
            k = k.astype(BF16)
            decays = jnp.where(lower, jnp.exp(jnp.where(lower, c_col - c_row, 0.0)), 0.0)
            weights = (dot(q, k, ((1,), (1,))) * decays).astype(BF16)
            qf = q.astype(F32)
            inner = dot(weights, v)
            if b:
                inner = inner + dot((qf * jnp.exp(c_col)).astype(BF16), states[h].astype(BF16))
            ret_ref[part, lanes] = inner
            qd_ref[part, lanes] = (qf * jnp.exp(c_col + base[h])).astype(BF16)
            scaled = (k.astype(F32) * jnp.exp(total - c_col)).astype(BF16)
            update = dot(scaled, v, ((0,), (0,)))
            states[h] = jnp.exp(total) * states[h] + update
            base[h] = base[h] + total
    span = head_dim + PAD
    peers = pkg_ref.shape[0]
    for h in range(heads):
        state = states[h].astype(BF16)
        factor = jnp.broadcast_to(jnp.exp(base[h]), (PAD, head_dim)).astype(BF16)
        pkg_ref[:, h * span : h * span + head_dim, :] = jnp.broadcast_to(
            state[None], (peers,) + state.shape
        )
        pkg_ref[:, h * span + head_dim : (h + 1) * span, :] = jnp.broadcast_to(
            factor[None], (peers,) + factor.shape
        )


def finish_kernel(index_ref, ret_ref, qd_ref, gate_ref, hgain_ref, wo_ref, pkg_ref, *refs, heads, head_dim):
    outs, hidden_ref = refs[:-1], refs[-1]
    pieces = len(outs)
    span = head_dim + PAD
    for h in range(heads):
        lanes = slice(h * head_dim, (h + 1) * head_dim)

        def turn(k, state, h=h):
            local = pkg_ref[k, h * span : h * span + head_dim, :].astype(F32)
            factor = pkg_ref[k, h * span + head_dim : (h + 1) * span, :].astype(F32)[0:1, :]
            return factor * state + local

        state = lax.fori_loop(0, index_ref[pieces], turn, jnp.zeros((head_dim, head_dim), F32))
        kept = ret_ref[:, lanes] + dot(qd_ref[:, lanes], state.astype(BF16))
        centre = jnp.mean(kept, axis=-1, keepdims=True)
        away = kept - centre
        spread = jnp.mean(away * away, axis=-1, keepdims=True)
        scaled = away * lax.rsqrt(spread + EPS) * hgain_ref[:, lanes]
        hidden_ref[:, lanes] = (scaled * silu(gate_ref[:, lanes].astype(F32))).astype(BF16)
    for j in reversed(range(pieces)):
        size = outs[j].shape[0]
        start = pl.multiple_of(index_ref[j] * size, size)
        outs[j][...] = dot(hidden_ref[pl.ds(start, size), :], wo_ref[...]).astype(BF16)


def dispatch_kernel(x_ref, gain_ref, routes_ref, weight_ref, out_ref, hi_ref, lo_ref, *, capacity):
    top, tokens = routes_ref.shape
    slots = out_ref.shape[0]
    experts = slots // capacity
    normed = normed_rows(x_ref[...], gain_ref[...])
    row_ids = lax.broadcasted_iota(jnp.int32, (tokens, tokens), 0)
    col_ids = lax.broadcasted_iota(jnp.int32, (tokens, tokens), 1)
    before = (row_ids < col_ids).astype(F32).astype(BF16)
    line = lax.broadcasted_iota(jnp.int32, (experts, tokens), 0)
    slot = lax.broadcasted_iota(jnp.int32, (slots, tokens), 0)
    routes = routes_ref[...]
    scores = weight_ref[...]
    share = scores / jnp.sum(scores, axis=0, keepdims=True)
    offset = jnp.zeros((experts, 1), F32)
    place = jnp.zeros((slots, tokens), F32)
    mix = jnp.zeros((slots, tokens), F32)
    for t in range(top):
        expert = routes[t : t + 1, :]
        onehot = (line == expert).astype(F32)
        prior = dot(onehot.astype(BF16), before) + offset
        position = jnp.sum(prior * onehot, axis=0, keepdims=True)
        target = expert * capacity + position.astype(jnp.int32)
        hit = (slot == target).astype(F32)
        place = place + hit
        mix = mix + hit * share[t : t + 1, :]
        offset = offset + jnp.sum(onehot, axis=1, keepdims=True)
    out_ref[...] = dot(place.astype(BF16), normed).astype(BF16)
    high = mix.astype(BF16)
    hi_ref[...] = high
    lo_ref[...] = (mix - high.astype(F32)).astype(BF16)


def gate_up_kernel(rows_ref, *refs, pieces):
    gates, ups = refs[:pieces], refs[pieces : 2 * pieces]
    out_ref, gacc_ref, uacc_ref = refs[2 * pieces :]
    step = pl.program_id(0)
    rows = rows_ref[...]
    width = gates[0].shape[1]

    @pl.when(step == 0)
    def _():
        gacc_ref[...] = jnp.zeros_like(gacc_ref)
        uacc_ref[...] = jnp.zeros_like(uacc_ref)

    for i in range(pieces):
        lanes = slice(i * width, (i + 1) * width)
        gacc_ref[:, lanes] += dot(rows, gates[i][...])
        uacc_ref[:, lanes] += dot(rows, ups[i][...])

    @pl.when(step == pl.num_programs(0) - 1)
    def _():
        out_ref[...] = (silu(gacc_ref[...]) * uacc_ref[...]).astype(BF16)


def gate_up(rows, gates, ups):
    count, width = rows.shape
    pieces, cols = len(gates), gates[0].shape[1]
    part = width // 4
    weight = pl.BlockSpec((part, cols), lambda i: (i, 0))
    return pl.pallas_call(
        functools.partial(gate_up_kernel, pieces=pieces),
        grid=(4,),
        in_specs=[pl.BlockSpec((count, part), lambda i: (0, i))] + [weight] * (2 * pieces),
        out_specs=pl.BlockSpec((count, pieces * cols), lambda i: (0, 0)),
        out_shape=jax.ShapeDtypeStruct((count, pieces * cols), BF16),
        scratch_shapes=[pltpu.VMEM((count, pieces * cols), F32)] * 2,
        name="gate_up",
    )(rows, *gates, *ups)


def down_kernel(*refs, groups):
    hiddens, downs, out_ref = refs[: len(groups)], refs[len(groups) : -1], refs[-1]
    total, at = None, 0
    for hidden, pieces in zip(hiddens, groups):
        cols = downs[at].shape[0]
        for i in range(pieces):
            term = dot(hidden[:, i * cols : (i + 1) * cols], downs[at][...])
            total = term if total is None else total + term
            at += 1
    out_ref[...] = total.astype(BF16)


def down(hiddens, groups):
    count = hiddens[0].shape[0]
    flat = [d for g in groups for d in g]
    inner, width = flat[0].shape
    part = width // 2
    return pl.pallas_call(
        functools.partial(down_kernel, groups=tuple(len(g) for g in groups)),
        grid=(2,),
        in_specs=[pl.BlockSpec(h.shape, lambda i: (0, 0)) for h in hiddens]
        + [pl.BlockSpec((inner, part), lambda i: (0, i))] * len(flat),
        out_specs=pl.BlockSpec((count, part), lambda i: (0, i)),
        out_shape=jax.ShapeDtypeStruct((count, width), BF16),
        name="down",
    )(*hiddens, *flat)


def combine_kernel(hi_ref, lo_ref, rows_ref, *refs):
    rows = rows_ref[...]
    first = ((0,), (0,))
    refs[-1][...] = (dot(hi_ref[...], rows, first) + dot(lo_ref[...], rows, first)).astype(BF16)


def combine(mix_hi, mix_lo, rows, at, width, before):
    slots, tokens = mix_hi.shape
    cols = rows.shape[1]
    part = cols // 2
    mix = pl.BlockSpec((slots, tokens), lambda i: (0, 0))
    in_specs = [mix, mix, pl.BlockSpec((slots, part), lambda i: (0, i))]
    operands = [mix_hi, mix_lo, rows]
    if before is not None:
        in_specs.append(pl.BlockSpec(memory_space=pl.ANY))
        operands.append(before)
    return pl.pallas_call(
        combine_kernel,
        grid=(2,),
        in_specs=in_specs,
        out_specs=pl.BlockSpec((tokens, part), lambda i: (0, i + 2 * at)),
        out_shape=jax.ShapeDtypeStruct((tokens, width), BF16),
        input_output_aliases={} if before is None else {3: 0},
        name="combine",
    )(*operands)


def swap(x, axis, bit):
    return lax.ppermute(x, axis, [(i, i ^ bit) for i in range(lax.axis_size(axis))])


def on_device(
    mixer_input,
    mixer_gain,
    query_weight,
    key_weight,
    value_weight,
    gate_weight,
    head_gain,
    output_weight,
    log_decay,
    expert_input,
    expert_gain,
    routes,
    route_weight,
    expert_gate,
    expert_up,
    expert_down,
):
    tp = lax.axis_size("tp")
    bits = []
    while (1 << len(bits)) < tp:
        bits.append(1 << len(bits))

    def spread(piece):
        pieces = [piece]
        for bit in reversed(bits):
            pieces = pieces + [swap(p, "tp", bit) for p in pieces]
        return pieces

    full = expert_down.shape[2]
    chunks = 2
    cut = full // chunks
    gates, ups = spread(expert_gate[0]), spread(expert_up[0])
    downs = [spread(expert_down[0][:, c * cut : (c + 1) * cut]) for c in range(chunks)]

    tokens, top = routes.shape
    experts = lax.axis_size("ep")
    capacity = max(2, 3 * tokens * top // (2 * experts))
    slots = experts * capacity
    width = expert_input.shape[1]
    outgoing, mix_hi, mix_lo = pl.pallas_call(
        functools.partial(dispatch_kernel, capacity=capacity),
        out_shape=(
            jax.ShapeDtypeStruct((slots, width), BF16),
            jax.ShapeDtypeStruct((slots, tokens), BF16),
            jax.ShapeDtypeStruct((slots, tokens), BF16),
        ),
        name="dispatch",
    )(expert_input, expert_gain.reshape(1, -1), routes.T, route_weight.T)
    arrived = lax.all_to_all(
        outgoing.reshape(experts, capacity, width), "ep", split_axis=0, concat_axis=0, tiled=True
    ).reshape(slots, width)

    rows = mixer_input.shape[0]
    heads = log_decay.shape[1]
    mix_width = query_weight.shape[1]
    head_dim = mix_width // heads
    half = head_dim // 2
    position = lax.axis_index("ep") * rows + jnp.arange(rows, dtype=jnp.int32)
    lane = jnp.arange(head_dim, dtype=jnp.int32)
    frequency = 10000.0 ** (-(lane % half).astype(F32) / half)
    angles = position.astype(F32)[:, None] * frequency[None, :]
    cosine = jnp.cos(angles)
    sine = jnp.where(lane < half, -1.0, 1.0)[None, :] * jnp.sin(angles)
    span = head_dim + PAD
    retained, queries, gate_raw, package = pl.pallas_call(
        functools.partial(retain_kernel, heads=heads, head_dim=head_dim),
        out_shape=(
            jax.ShapeDtypeStruct((rows, mix_width), F32),
            jax.ShapeDtypeStruct((rows, mix_width), BF16),
            jax.ShapeDtypeStruct((rows, mix_width), BF16),
            jax.ShapeDtypeStruct((experts, heads * span, head_dim), BF16),
        ),
        scratch_shapes=[pltpu.VMEM(mixer_input.shape, BF16)],
        name="retain",
    )(
        mixer_input,
        mixer_gain.reshape(1, -1),
        query_weight,
        key_weight,
        value_weight,
        gate_weight,
        cosine,
        sine,
        log_decay.T,
    )
    arrived, package = lax.optimization_barrier((arrived, package))
    packages = lax.all_to_all(package, "ep", split_axis=0, concat_axis=0, tiled=True)
    out_width = output_weight.shape[1]
    order = lax.axis_index("tp") ^ jnp.arange(tp + 1, dtype=jnp.int32)
    order = jnp.where(jnp.arange(tp + 1) < tp, order, lax.axis_index("ep")).astype(jnp.int32)
    vmem = pl.BlockSpec(memory_space=pltpu.VMEM)
    parts = pl.pallas_call(
        functools.partial(finish_kernel, heads=heads, head_dim=head_dim),
        in_specs=[pl.BlockSpec(memory_space=pltpu.SMEM)] + [vmem] * 6,
        out_specs=[vmem] * tp,
        out_shape=[jax.ShapeDtypeStruct((rows // tp, out_width), BF16)] * tp,
        scratch_shapes=[pltpu.VMEM((rows, mix_width), BF16)],
        name="finish",
    )(order, retained, queries, gate_raw, head_gain.reshape(1, -1), output_weight, packages)
    sums = [part for part in parts]
    for bit in bits:
        kept = range(0, len(sums), 2 * bit)
        for j in kept:
            other = swap(sums[j + bit].astype(BF16), "tp", bit)
            sums[j] = sums[j].astype(F32) + other.astype(F32)
    mixer_output = sums[0].astype(BF16)

    near, far = slice(0, None, 2), slice(1, None, 2)
    if tp > 2:
        split = [near, far]
    else:
        split = [slice(0, None)]
    hiddens = [gate_up(arrived, gates[s], ups[s]) for s in split]
    hiddens = list(lax.optimization_barrier((tuple(hiddens), parts[-1]))[0])
    expert_output = None
    for c in range(chunks):
        results = down(hiddens, [downs[c][s] for s in split])
        returned = lax.all_to_all(
            results.reshape(experts, capacity, cut), "ep", split_axis=0, concat_axis=0, tiled=True
        ).reshape(slots, cut)
        expert_output = combine(mix_hi, mix_lo, returned, c, full, expert_output)
    return (mixer_output, expert_output)


def solution(mesh):
    return jax.shard_map(
        on_device,
        mesh=mesh,
        in_specs=(
            P("ep", None),
            P(),
            P(None, "tp"),
            P(None, "tp"),
            P(None, "tp"),
            P(None, "tp"),
            P("tp"),
            P("tp", None),
            P("ep", "tp"),
            P(("ep", "tp"), None),
            P(),
            P(("ep", "tp"), None),
            P(("ep", "tp"), None),
            P("ep", None, "tp"),
            P("ep", None, "tp"),
            P("ep", "tp", None),
        ),
        out_specs=(P(("ep", "tp"), None), P(("ep", "tp"), None)),
        check_vma=False,
    )
```

```python
import functools

import jax
import jax.numpy as jnp
from jax import lax
from jax.experimental import pallas as pl
from jax.experimental.pallas import tpu as pltpu
from jax.sharding import PartitionSpec as P


BLOCK = 128
EPS = 1e-06
HIGH = lax.Precision.HIGHEST
PAD = 16
F32 = jnp.float32
BF16 = jnp.bfloat16


def dot(a, b, contract=((1,), (0,)), precision=None):
    return lax.dot_general(
        a, b, (contract, ((), ())), preferred_element_type=F32, precision=precision
    )


def normed_rows(values, gain):
    floats = values.astype(F32)
    scale = lax.rsqrt(jnp.mean(floats * floats, axis=-1, keepdims=True) + EPS)
    return (floats * scale * gain).astype(BF16)


def silu(v):
    return v / (1.0 + jnp.exp(-v))


def retain_kernel(
    x_ref,
    gain_ref,
    wq_ref,
    wk_ref,
    wv_ref,
    wg_ref,
    cos_ref,
    sin_ref,
    ldt_ref,
    ret_ref,
    qd_ref,
    gate_ref,
    pkg_ref,
    normed_ref,
    *,
    heads,
    head_dim,
):
    rows = x_ref.shape[0]
    blocks = rows // BLOCK
    for b in range(blocks):
        part = slice(b * BLOCK, (b + 1) * BLOCK)
        normed_ref[part, :] = normed_rows(x_ref[part, :], gain_ref[...])
    normed = normed_ref[...]
    q_all = dot(normed, wq_ref[...]).astype(BF16)
    k_all = dot(normed, wk_ref[...]).astype(BF16)
    v_all = dot(normed, wv_ref[...]).astype(BF16)
    gate_ref[...] = dot(normed, wg_ref[...]).astype(BF16)
    row_ids = lax.broadcasted_iota(jnp.int32, (BLOCK, BLOCK), 0)
    col_ids = lax.broadcasted_iota(jnp.int32, (BLOCK, BLOCK), 1)
    lower = col_ids <= row_ids
    tri = lower.astype(F32)
    tri_t = (row_ids <= col_ids).astype(F32)
    states = [jnp.zeros((head_dim, head_dim), F32) for _ in range(heads)]
    base = [jnp.zeros((1, 1), F32) for _ in range(heads)]
    for b in range(blocks):
        part = slice(b * BLOCK, (b + 1) * BLOCK)
        c_cols = dot(tri, ldt_ref[:, part], ((1,), (1,)), precision=HIGH)
        c_rows = dot(ldt_ref[:, part], tri_t, precision=HIGH)
        cosine, sine = cos_ref[part, :], sin_ref[part, :]
        for h in range(heads):
            lanes = slice(h * head_dim, (h + 1) * head_dim)
            c_col = c_cols[:, h : h + 1]
            c_row = c_rows[h : h + 1, :]
            total = c_row[:, BLOCK - 1 : BLOCK]
            q = q_all[part, lanes].astype(F32)
            k = k_all[part, lanes].astype(F32)
            v = v_all[part, lanes]
            q = (q * cosine + pltpu.roll(q, head_dim // 2, 1) * sine).astype(BF16)
            k = (k * cosine + pltpu.roll(k, head_dim // 2, 1) * sine) * head_dim ** (-0.5)
            k = k.astype(BF16)
            decays = jnp.where(lower, jnp.exp(jnp.where(lower, c_col - c_row, 0.0)), 0.0)
            weights = (dot(q, k, ((1,), (1,))) * decays).astype(BF16)
            qf = q.astype(F32)
            inner = dot(weights, v)
            if b:
                inner = inner + dot((qf * jnp.exp(c_col)).astype(BF16), states[h].astype(BF16))
            ret_ref[part, lanes] = inner
            qd_ref[part, lanes] = (qf * jnp.exp(c_col + base[h])).astype(BF16)
            scaled = (k.astype(F32) * jnp.exp(total - c_col)).astype(BF16)
            update = dot(scaled, v, ((0,), (0,)))
            states[h] = jnp.exp(total) * states[h] + update
            base[h] = base[h] + total
    span = head_dim + PAD
    peers = pkg_ref.shape[0]
    for h in range(heads):
        state = states[h].astype(BF16)
        factor = jnp.broadcast_to(jnp.exp(base[h]), (PAD, head_dim)).astype(BF16)
        pkg_ref[:, h * span : h * span + head_dim, :] = jnp.broadcast_to(
            state[None], (peers,) + state.shape
        )
        pkg_ref[:, h * span + head_dim : (h + 1) * span, :] = jnp.broadcast_to(
            factor[None], (peers,) + factor.shape
        )


def finish_kernel(index_ref, ret_ref, qd_ref, gate_ref, hgain_ref, wo_ref, pkg_ref, *refs, heads, head_dim):
    outs, hidden_ref = refs[:-1], refs[-1]
    pieces = len(outs)
    span = head_dim + PAD
    for h in range(heads):
        lanes = slice(h * head_dim, (h + 1) * head_dim)

        def turn(k, state, h=h):
            local = pkg_ref[k, h * span : h * span + head_dim, :].astype(F32)
            factor = pkg_ref[k, h * span + head_dim : (h + 1) * span, :].astype(F32)[0:1, :]
            return factor * state + local

        state = lax.fori_loop(0, index_ref[pieces], turn, jnp.zeros((head_dim, head_dim), F32))
        kept = ret_ref[:, lanes] + dot(qd_ref[:, lanes], state.astype(BF16))
        centre = jnp.mean(kept, axis=-1, keepdims=True)
        away = kept - centre
        spread = jnp.mean(away * away, axis=-1, keepdims=True)
        scaled = away * lax.rsqrt(spread + EPS) * hgain_ref[:, lanes]
        hidden_ref[:, lanes] = (scaled * silu(gate_ref[:, lanes].astype(F32))).astype(BF16)
    for j in reversed(range(pieces)):
        size = outs[j].shape[0]
        start = pl.multiple_of(index_ref[j] * size, size)
        outs[j][...] = dot(hidden_ref[pl.ds(start, size), :], wo_ref[...]).astype(BF16)


def dispatch_kernel(x_ref, gain_ref, routes_ref, weight_ref, out_ref, hi_ref, lo_ref, *, capacity):
    top, tokens = routes_ref.shape
    slots = out_ref.shape[0]
    experts = slots // capacity
    normed = normed_rows(x_ref[...], gain_ref[...])
    row_ids = lax.broadcasted_iota(jnp.int32, (tokens, tokens), 0)
    col_ids = lax.broadcasted_iota(jnp.int32, (tokens, tokens), 1)
    before = (row_ids < col_ids).astype(F32).astype(BF16)
    line = lax.broadcasted_iota(jnp.int32, (experts, tokens), 0)
    slot = lax.broadcasted_iota(jnp.int32, (slots, tokens), 0)
    routes = routes_ref[...]
    scores = weight_ref[...]
    share = scores / jnp.sum(scores, axis=0, keepdims=True)
    offset = jnp.zeros((experts, 1), F32)
    place = jnp.zeros((slots, tokens), F32)
    mix = jnp.zeros((slots, tokens), F32)
    for t in range(top):
        expert = routes[t : t + 1, :]
        onehot = (line == expert).astype(F32)
        prior = dot(onehot.astype(BF16), before) + offset
        position = jnp.sum(prior * onehot, axis=0, keepdims=True)
        target = expert * capacity + position.astype(jnp.int32)
        hit = (slot == target).astype(F32)
        place = place + hit
        mix = mix + hit * share[t : t + 1, :]
        offset = offset + jnp.sum(onehot, axis=1, keepdims=True)
    out_ref[...] = dot(place.astype(BF16), normed).astype(BF16)
    high = mix.astype(BF16)
    hi_ref[...] = high
    lo_ref[...] = (mix - high.astype(F32)).astype(BF16)


def gate_up_kernel(rows_ref, *refs, pieces):
    gates, ups = refs[:pieces], refs[pieces : 2 * pieces]
    out_ref, gacc_ref, uacc_ref = refs[2 * pieces :]
    step = pl.program_id(0)
    rows = rows_ref[...]
    width = gates[0].shape[1]

    @pl.when(step == 0)
    def _():
        gacc_ref[...] = jnp.zeros_like(gacc_ref)
        uacc_ref[...] = jnp.zeros_like(uacc_ref)

    for i in range(pieces):
        lanes = slice(i * width, (i + 1) * width)
        gacc_ref[:, lanes] += dot(rows, gates[i][...])
        uacc_ref[:, lanes] += dot(rows, ups[i][...])

    @pl.when(step == pl.num_programs(0) - 1)
    def _():
        out_ref[...] = (silu(gacc_ref[...]) * uacc_ref[...]).astype(BF16)


def gate_up(rows, gates, ups):
    count, width = rows.shape
    pieces, cols = len(gates), gates[0].shape[1]
    part = width // 4
    weight = pl.BlockSpec((part, cols), lambda i: (i, 0))
    return pl.pallas_call(
        functools.partial(gate_up_kernel, pieces=pieces),
        grid=(4,),
        in_specs=[pl.BlockSpec((count, part), lambda i: (0, i))] + [weight] * (2 * pieces),
        out_specs=pl.BlockSpec((count, pieces * cols), lambda i: (0, 0)),
        out_shape=jax.ShapeDtypeStruct((count, pieces * cols), BF16),
        scratch_shapes=[pltpu.VMEM((count, pieces * cols), F32)] * 2,
        name="gate_up",
    )(rows, *gates, *ups)


def down_kernel(*refs, groups):
    hiddens, downs, out_ref = refs[: len(groups)], refs[len(groups) : -1], refs[-1]
    total, at = None, 0
    for hidden, pieces in zip(hiddens, groups):
        cols = downs[at].shape[0]
        for i in range(pieces):
            term = dot(hidden[:, i * cols : (i + 1) * cols], downs[at][...])
            total = term if total is None else total + term
            at += 1
    out_ref[...] = total.astype(BF16)


def down(hiddens, groups):
    count = hiddens[0].shape[0]
    flat = [d for g in groups for d in g]
    inner, width = flat[0].shape
    part = width // 2
    return pl.pallas_call(
        functools.partial(down_kernel, groups=tuple(len(g) for g in groups)),
        grid=(2,),
        in_specs=[pl.BlockSpec(h.shape, lambda i: (0, 0)) for h in hiddens]
        + [pl.BlockSpec((inner, part), lambda i: (0, i))] * len(flat),
        out_specs=pl.BlockSpec((count, part), lambda i: (0, i)),
        out_shape=jax.ShapeDtypeStruct((count, width), BF16),
        name="down",
    )(*hiddens, *flat)


def combine(mix_hi, mix_lo, rows):
    first = ((0,), (0,))
    return (dot(mix_hi, rows, first) + dot(mix_lo, rows, first)).astype(BF16)


def swap(x, axis, bit):
    return lax.ppermute(x, axis, [(i, i ^ bit) for i in range(lax.axis_size(axis))])


def on_device(
    mixer_input,
    mixer_gain,
    query_weight,
    key_weight,
    value_weight,
    gate_weight,
    head_gain,
    output_weight,
    log_decay,
    expert_input,
    expert_gain,
    routes,
    route_weight,
    expert_gate,
    expert_up,
    expert_down,
):
    tp = lax.axis_size("tp")
    bits = []
    while (1 << len(bits)) < tp:
        bits.append(1 << len(bits))

    def spread(piece):
        pieces = [piece]
        for bit in reversed(bits):
            pieces = pieces + [swap(p, "tp", bit) for p in pieces]
        return pieces

    full = expert_down.shape[2]
    chunks = 2
    cut = full // chunks
    gates, ups = spread(expert_gate[0]), spread(expert_up[0])
    downs = [spread(expert_down[0][:, c * cut : (c + 1) * cut]) for c in range(chunks)]

    tokens, top = routes.shape
    experts = lax.axis_size("ep")
    capacity = max(2, 3 * tokens * top // (2 * experts))
    slots = experts * capacity
    width = expert_input.shape[1]
    outgoing, mix_hi, mix_lo = pl.pallas_call(
        functools.partial(dispatch_kernel, capacity=capacity),
        out_shape=(
            jax.ShapeDtypeStruct((slots, width), BF16),
            jax.ShapeDtypeStruct((slots, tokens), BF16),
            jax.ShapeDtypeStruct((slots, tokens), BF16),
        ),
        name="dispatch",
    )(expert_input, expert_gain.reshape(1, -1), routes.T, route_weight.T)
    arrived = lax.all_to_all(
        outgoing.reshape(experts, capacity, width), "ep", split_axis=0, concat_axis=0, tiled=True
    ).reshape(slots, width)

    rows = mixer_input.shape[0]
    heads = log_decay.shape[1]
    mix_width = query_weight.shape[1]
    head_dim = mix_width // heads
    half = head_dim // 2
    position = lax.axis_index("ep") * rows + jnp.arange(rows, dtype=jnp.int32)
    lane = jnp.arange(head_dim, dtype=jnp.int32)
    frequency = 10000.0 ** (-(lane % half).astype(F32) / half)
    angles = position.astype(F32)[:, None] * frequency[None, :]
    cosine = jnp.cos(angles)
    sine = jnp.where(lane < half, -1.0, 1.0)[None, :] * jnp.sin(angles)
    span = head_dim + PAD
    retained, queries, gate_raw, package = pl.pallas_call(
        functools.partial(retain_kernel, heads=heads, head_dim=head_dim),
        out_shape=(
            jax.ShapeDtypeStruct((rows, mix_width), F32),
            jax.ShapeDtypeStruct((rows, mix_width), BF16),
            jax.ShapeDtypeStruct((rows, mix_width), BF16),
            jax.ShapeDtypeStruct((experts, heads * span, head_dim), BF16),
        ),
        scratch_shapes=[pltpu.VMEM(mixer_input.shape, BF16)],
        name="retain",
    )(
        mixer_input,
        mixer_gain.reshape(1, -1),
        query_weight,
        key_weight,
        value_weight,
        gate_weight,
        cosine,
        sine,
        log_decay.T,
    )
    arrived, package = lax.optimization_barrier((arrived, package))
    packages = lax.all_to_all(package, "ep", split_axis=0, concat_axis=0, tiled=True)
    near, far = slice(0, None, 2), slice(1, None, 2)
    if tp > 2:
        split = [near, far]
    else:
        split = [slice(0, None)]
    hiddens = []
    for part in split:
        hiddens.append(gate_up(arrived, gates[part], ups[part]))
    first = down(hiddens, [downs[0][part] for part in split])
    packages = lax.optimization_barrier((packages, first))[0]

    out_width = output_weight.shape[1]
    order = lax.axis_index("tp") ^ jnp.arange(tp + 1, dtype=jnp.int32)
    order = jnp.where(jnp.arange(tp + 1) < tp, order, lax.axis_index("ep")).astype(jnp.int32)
    vmem = pl.BlockSpec(memory_space=pltpu.VMEM)
    parts = pl.pallas_call(
        functools.partial(finish_kernel, heads=heads, head_dim=head_dim),
        in_specs=[pl.BlockSpec(memory_space=pltpu.SMEM)] + [vmem] * 6,
        out_specs=[vmem] * tp,
        out_shape=[jax.ShapeDtypeStruct((rows // tp, out_width), BF16)] * tp,
        scratch_shapes=[pltpu.VMEM((rows, mix_width), BF16)],
        name="finish",
    )(order, retained, queries, gate_raw, head_gain.reshape(1, -1), output_weight, packages)
    sums = [part for part in parts]
    for bit in bits:
        kept = range(0, len(sums), 2 * bit)
        for j in kept:
            other = swap(sums[j + bit].astype(BF16), "tp", bit)
            sums[j] = sums[j].astype(F32) + other.astype(F32)
    mixer_output = sums[0].astype(BF16)

    hiddens = list(lax.optimization_barrier((tuple(hiddens), parts[-1]))[0])
    columns = []
    for c in range(chunks):
        results = down(hiddens, [downs[c][part] for part in split]) if c else first
        returned = lax.all_to_all(
            results.reshape(experts, capacity, cut), "ep", split_axis=0, concat_axis=0, tiled=True
        ).reshape(slots, cut)
        columns.append(combine(mix_hi, mix_lo, returned))
    expert_output = jnp.concatenate(columns, axis=1)
    return (mixer_output, expert_output)


def solution(mesh):
    return jax.shard_map(
        on_device,
        mesh=mesh,
        in_specs=(
            P("ep", None),
            P(),
            P(None, "tp"),
            P(None, "tp"),
            P(None, "tp"),
            P(None, "tp"),
            P("tp"),
            P("tp", None),
            P("ep", "tp"),
            P(("ep", "tp"), None),
            P(),
            P(("ep", "tp"), None),
            P(("ep", "tp"), None),
            P("ep", None, "tp"),
            P("ep", None, "tp"),
            P("ep", "tp", None),
        ),
        out_specs=(P(("ep", "tp"), None), P(("ep", "tp"), None)),
        check_vma=False,
    )
```
